32 devices in a mesh: kv: 16 (over z, y, x), tp: 2 (over core).
Axes of the slice: x: 2, y: 2, z: 4, core: 2. Of those that a mesh axis runs over, the one named last changes fastest.
Arguments:
- normed: bfloat16 [8192, 4096], P('kv'), may hold values from -6 to 6
- queries: bfloat16 [8192, 1024], P('kv', 'tp'), may hold values from -6 to 6
- keys: bfloat16 [8192, 64], P('kv'), may hold values from -6 to 6
- values: bfloat16 [8192, 64], P('kv'), may hold values from -6 to 6
- attended: bfloat16 [8192, 1024], P('kv', 'tp'), may hold values from -6 to 6
- cotangent: bfloat16 [8192, 1024], P('kv', 'tp'), may hold values from -24 to 24
- log_sum: float32 [8192, 16], P('kv', 'tp'), may hold values from 6 to 8
- chosen: int32 [128, 16], P('kv'), may hold values from -1 to 127, as said below
Outputs:
- grad_queries: bfloat16 [8192, 1024], P('kv', 'tp')
- grad_keys: float32 [8192, 64], P('kv')
- grad_values: float32 [8192, 64], P('kv')
- weight_grad: float32 [4096, 1024], P('kv', 'tp')
The draws below stay inside these ranges and needn't reach their ends.
Inputs may be any that keep to these rules, and one draw needn't show every extreme that they name: `chosen`: each row lists distinct key blocks, none after its own block, and always its own block; the listed entries come first and -1 fills the rest. A row lists from 8 to 16 blocks, fewer only where fewer blocks are open to it; on every index of kv some row lists 16 blocks where that many are open. The rows of one index of kv together list at most one block of each other index of kv's positions; every index of kv from 1 on lists a block of index 0 and a block of the index before it, and every index from half the axis on a block of the index half the axis before it.
All inputs are finite; a program needn't handle non-finite values.
Results may differ from the reference program's by a relative error of at most 0.007.
Values may be sent and summed in bfloat16 or wider, within the bound.
No kernel may reach another device: no remote copies, remote signals or barrier semaphores. Data moves between devices by JAX's collectives and lax.ppermute only.
A program may use at most 64 MiB of HBM per device.

```python
import jax
import jax.numpy as jnp
from jax import lax

D = 4096
HEADS = 16
HEAD_DIM = 64
BLOCK = 64
NSEL = 16
LEAST = 8
TOK_DEV = 512
TOKENS = 8192


def draw_chosen(key, part):
    device_count = TOKENS // TOK_DEV
    per_device = TOK_DEV // BLOCK
    block_count = TOKENS // BLOCK
    first_key = jax.random.fold_in(key, 11)
    second_key = jax.random.fold_in(key, 12)
    third_key = jax.random.fold_in(key, 13)
    fourth_key = jax.random.fold_in(key, 14)
    offsets = jax.random.randint(first_key, (device_count, device_count), 0, per_device)
    row_ids = jnp.arange(block_count, dtype=jnp.int32)
    col_ids = jnp.arange(block_count, dtype=jnp.int32)
    row_dev = row_ids // per_device
    col_dev = col_ids // per_device
    fetched = col_dev[None, :] * per_device + offsets[row_dev[:, None], col_dev[None, :]]
    local_open = (col_dev[None, :] == row_dev[:, None]) & (col_ids[None, :] <= row_ids[:, None])
    remote_open = (col_dev[None, :] < row_dev[:, None]) & (col_ids[None, :] == fetched)
    is_open = local_open | remote_open
    near = (col_dev[None, :] == row_dev[:, None] - 1) | (col_dev[None, :] == row_dev[:, None] - device_count // 2) | (col_dev[None, :] == 0)
    forced = (col_ids[None, :] == row_ids[:, None]) | remote_open & near
    noise = jax.random.randint(second_key, (block_count, block_count), 0, 4096)
    ranked = jnp.where(forced, 2 ** 28 + col_ids[None, :], jnp.where(is_open, noise * block_count + col_ids[None, :], -1 - col_ids[None, :]))
    top_values, picked = lax.top_k(ranked, NSEL)
    span_size = NSEL - LEAST + 1
    first_draw = jax.random.randint(third_key, (block_count,), 0, span_size)
    second_draw = jax.random.randint(fourth_key, (block_count,), 0, span_size)
    listed_count = LEAST + jnp.minimum(first_draw, second_draw)
    listed_count = jnp.where(row_ids % per_device == per_device - 1, NSEL, listed_count)
    slot_ids = jnp.arange(NSEL, dtype=jnp.int32)
    keep = (slot_ids[None, :] < listed_count[:, None]) & (top_values >= 0)
    return jnp.where(keep, picked, -1).astype(jnp.int32)


def strengthened(entries, stream_key, source, target, blocks, factor):
    def block_of(dim):
        return (jnp.arange(entries.shape[dim]) // (entries.shape[dim] // blocks)).reshape((-1,) + (1,) * (entries.ndim - 1 - dim))

    first = jax.random.permutation(stream_key, blocks)[block_of(target)]
    other_side = (block_of(target) + blocks // 2) % blocks
    return jnp.where((block_of(source) == first) | (block_of(source) == other_side), factor * entries, entries)


def block_levels(key, shape, pieces, smallest, largest):
    level = 1.0
    for position, blocks in pieces:
        heights = jax.random.uniform(jax.random.fold_in(jax.random.fold_in(key, 6), position), (blocks,), jnp.float32, smallest / len(pieces), largest / len(pieces))
        level = level * jnp.repeat(jnp.exp(heights), shape[position] // blocks).reshape((-1,) + (1,) * (len(shape) - 1 - position))
    return level


def scatter_about(stream_key, extent, scale, reach, shards=(), kind=jnp.bfloat16):
    entries = jax.random.normal(stream_key, extent, jnp.float32) * scale
    if len(shards) > 0:
        entries = block_levels(stream_key, extent, shards, -0.22, 0.18) * entries
    return jnp.clip(entries, min=-reach, max=reach).astype(kind)


def noise_with(stream_key, shape, deviation, reach, cuts, heavy, held_as=jnp.bfloat16):
    values = deviation * jax.random.normal(stream_key, shape, jnp.float32)
    if cuts:
        values = values * block_levels(stream_key, shape, cuts, -0.22, 0.18)
    return jnp.clip(strengthened(values, jax.random.fold_in(stream_key, 3), *heavy), -reach, reach).astype(held_as)


def setup_inputs(seed: int = 0) -> dict:
    key_list = jax.random.split(jax.random.key(seed), 9)
    normed = noise_with(key_list[0], (TOKENS, D), 1.0, 6.0, ((0, 16),), (0, 1, 16, 2.0))
    queries = scatter_about(key_list[1], (TOKENS, HEADS * HEAD_DIM), 1.0, 6.0, ((0, 16), (1, 2)))
    keys = scatter_about(key_list[2], (TOKENS, HEAD_DIM), 1.0, 6.0, ((0, 16),))
    values = scatter_about(key_list[3], (TOKENS, HEAD_DIM), 1.0, 6.0, ((0, 16),))
    attended = scatter_about(key_list[4], (TOKENS, HEADS * HEAD_DIM), 1.0, 6.0, ((0, 16), (1, 2)))
    cotangent = scatter_about(key_list[5], (TOKENS, HEADS * HEAD_DIM), 4.0, 24.0, ((0, 16), (1, 2)))
    log_sum = jnp.clip(6.0 + 2.0 * jax.random.uniform(key_list[6], (TOKENS, HEADS), jnp.float32) ** block_levels(key_list[6], (TOKENS, HEADS), ((0, 16), (1, 2)), -0.2, 0.2), 6.0, 8.0)
    chosen = draw_chosen(jax.random.fold_in(key_list[8], 71), 0)
    return {"normed": normed, "queries": queries, "keys": keys, "values": values, "attended": attended, "cotangent": cotangent, "log_sum": log_sum, "chosen": chosen}


def reference(normed, queries, keys, values, attended, cotangent, log_sum, chosen):
    block_count = TOKENS // BLOCK
    score_scale = HEAD_DIM ** -0.5
    query_matrix = queries.reshape(block_count, BLOCK, HEADS, HEAD_DIM)
    gradient_rows = cotangent.reshape(block_count, BLOCK, HEADS, HEAD_DIM)
    out_rows = attended.reshape(block_count, BLOCK, HEADS, HEAD_DIM)
    log_rows = log_sum.reshape(block_count, BLOCK, HEADS)
    pair_rows = jnp.concatenate([keys, values], axis=1).reshape(block_count, BLOCK, 2 * HEAD_DIM)
    offsets = jnp.arange(BLOCK, dtype=jnp.int32)

    def one_block(accumulated, block_id):
        listed_ids = chosen[block_id]
        listed = listed_ids >= 0
        safe_ids = jnp.where(listed, listed_ids, 0).astype(jnp.int32)
        picked = pair_rows[safe_ids].reshape(NSEL * BLOCK, 2 * HEAD_DIM).astype(jnp.float32)
        selected_keys = picked[:, :HEAD_DIM]
        selected_values = picked[:, HEAD_DIM:]
        query_block = query_matrix[block_id].astype(jnp.float32)
        grad_block = gradient_rows[block_id].astype(jnp.float32)
        out_block = out_rows[block_id].astype(jnp.float32)
        key_pos = (safe_ids[:, None] * BLOCK + offsets[None, :]).reshape(NSEL * BLOCK)
        key_live = jnp.repeat(listed, BLOCK)
        query_pos = block_id * BLOCK + offsets
        allowed = key_live[None, :] & (key_pos[None, :] <= query_pos[:, None])
        scores = jnp.einsum('thd,kd->htk', query_block, selected_keys) * score_scale
        probs = jnp.where(allowed[None], jnp.exp(scores - log_rows[block_id].T[:, :, None]), 0.0)
        reduced_probabilities = lax.optimization_barrier(probs.astype(jnp.bfloat16)).astype(jnp.float32)
        grad_value = jnp.einsum('htk,thd->kd', reduced_probabilities, grad_block)
        probability_gradient = jnp.einsum('thd,kd->htk', grad_block, selected_values)
        deltas = jnp.sum(grad_block * out_block, axis=-1).T
        score_gradient = (probs * (probability_gradient - deltas[:, :, None]) * score_scale).astype(jnp.bfloat16)
        dscores_wide = lax.optimization_barrier(score_gradient).astype(jnp.float32)
        query_gradient = jnp.einsum('htk,kd->thd', dscores_wide, selected_keys).astype(jnp.bfloat16)
        key_gradient = jnp.einsum('htk,thd->kd', dscores_wide, query_block)
        terms = jnp.concatenate([key_gradient, grad_value], axis=1).reshape(NSEL, BLOCK, 2 * HEAD_DIM)
        terms = jnp.where(listed[:, None, None], terms, 0.0)
        accumulated = accumulated.at[safe_ids].add(terms)
        return accumulated, query_gradient.reshape(BLOCK, HEADS * HEAD_DIM)

    initial = jnp.zeros((block_count, BLOCK, 2 * HEAD_DIM), jnp.float32)
    accumulated, grad_blocks = lax.scan(one_block, initial, jnp.arange(block_count, dtype=jnp.int32))
    grad_queries = grad_blocks.reshape(TOKENS, HEADS * HEAD_DIM)
    grad_keys = accumulated[:, :, :HEAD_DIM].reshape(TOKENS, HEAD_DIM)
    grad_values = accumulated[:, :, HEAD_DIM:].reshape(TOKENS, HEAD_DIM)
    weight_grad = jnp.dot(normed.T, grad_queries, preferred_element_type=jnp.float32)
    return grad_queries, grad_keys, grad_values, weight_grad
```

```python
import functools
import math

import jax
import jax.numpy as jnp
from jax import lax
from jax.experimental import pallas as pl
from jax.experimental.pallas import tpu as pltpu
from jax.sharding import PartitionSpec as P

BLOCK = 64


def flat_perm(kv_of, tp_of=lambda core: core):
    kv_size, tp_size = lax.axis_size("kv"), lax.axis_size("tp")
    return [
        (kv * tp_size + tp, kv_of(kv) * tp_size + tp_of(tp))
        for kv in range(kv_size)
        for tp in range(tp_size)
    ]


def send(value, perm):
    return lax.ppermute(value, ("kv", "tp"), perm)


def group_size():
    kv_size = lax.axis_size("kv")
    return 4 if kv_size % 4 == 0 else 2 if kv_size % 2 == 0 else 1


def step_perm(step, size, stride):
    if size & (size - 1) == 0:
        return lambda kv: kv ^ (step * stride)
    base = size * stride
    return lambda kv: kv // base * base + (kv % base + step * stride) % base


def partner(index, step, size):
    return index ^ step if size & (size - 1) == 0 else (index + step) % size


def source(index, step, size):
    return index ^ step if size & (size - 1) == 0 else (index - step) % size


def columns_of(normed, member, group, first, rows):
    kv_size = lax.axis_size("kv")
    width = normed.shape[1] // kv_size
    parts = [
        lax.dynamic_slice(normed, (first, (outer * group + member) * width), (rows, width))
        for outer in range(kv_size // group)
    ]
    return jnp.concatenate(parts, axis=1)


def regroup_normed(normed):
    group = group_size()
    tp_size = lax.axis_size("tp")
    member = lax.axis_index("kv") % group
    rows = normed.shape[0]
    shares = 2 if tp_size % 2 == 0 else 1
    share = lax.axis_index("tp") % shares
    part = rows // shares
    mine = columns_of(normed, member, group, 0, rows)
    got = []
    for step in range(1, group):
        piece = columns_of(normed, partner(member, step, group), group, share * part, part)
        got.append(send(piece, flat_perm(step_perm(step, group, 1))))
    if shares == 1 or not got:
        return got, mine
    got = jnp.stack(got)
    other = send(got, flat_perm(lambda kv: kv, lambda tp: tp ^ 1))
    low = jnp.where(share == 0, got, other)
    high = jnp.where(share == 0, other, got)
    return [jnp.concatenate([low[i], high[i]], axis=0) for i in range(group - 1)], mine


def weight_gradient(moved, mine, query_gradient):
    group = group_size()
    kv_size = lax.axis_size("kv")
    outer = kv_size // group
    place = lax.axis_index("kv") // group
    others = [
        send(query_gradient, flat_perm(step_perm(step, group, 1))) for step in range(1, group)
    ]
    left = jnp.concatenate([mine] + moved, axis=0)
    right = jnp.concatenate([query_gradient] + others, axis=0)
    partial = lax.dot_general(
        left, right, (((0,), (0,)), ((), ())), preferred_element_type=jnp.float32
    )
    width = partial.shape[0] // outer
    narrow = partial.astype(jnp.bfloat16)
    total = lax.dynamic_slice_in_dim(partial, place * width, width, axis=0)
    for step in range(1, outer):
        piece = lax.dynamic_slice_in_dim(
            narrow, partner(place, step, outer) * width, width, axis=0
        )
        total = total + send(piece, flat_perm(step_perm(step, outer, group))).astype(jnp.float32)
    return total


def sum_over_tp(value):
    tp_size = lax.axis_size("tp")
    step = 1
    if tp_size & (tp_size - 1):
        return lax.psum(value, "tp")
    while step < tp_size:
        value = value + send(value, flat_perm(lambda kv: kv, lambda tp: tp ^ step))
        step *= 2
    return value


def by_parity(rows, blocks, heads):
    rows = rows.reshape(blocks, BLOCK, heads // 2, 2).transpose(0, 3, 2, 1)
    return rows.reshape(blocks, 1, heads * BLOCK)


def attention_kernel(
    slots_at_once, head_dim, slot_ref, limit_ref, rounds_ref, q_ref, d_ref, lse_ref, delta_ref,
    table_ref, dq_ref, sums_ref, stack_ref, dq_t_ref,
):
    block = pl.program_id(0)
    width = lse_ref.shape[2]
    pairs = q_ref.shape[1] // (2 * head_dim)
    score_scale = head_dim ** (-0.5)

    @pl.when(block == 0)
    def _():
        sums_ref[...] = jnp.zeros_like(sums_ref)

    low = lax.broadcasted_iota(jnp.int32, (BLOCK, 2 * head_dim), 1) < head_dim
    for pair in range(pairs):
        columns = slice(pair * 2 * head_dim, (pair + 1) * 2 * head_dim)
        query = q_ref[:, columns].astype(jnp.float32)
        grad = d_ref[:, columns].astype(jnp.float32)
        even = pl.ds(pair * BLOCK, BLOCK)
        odd = pl.ds((pairs + pair) * BLOCK, BLOCK)
        even_grad = pl.ds((2 * pairs + pair) * BLOCK, BLOCK)
        odd_grad = pl.ds((3 * pairs + pair) * BLOCK, BLOCK)
        turned = pltpu.roll(query, head_dim, 1)
        turned_grad = pltpu.roll(grad, head_dim, 1)
        stack_ref[even, :] = jnp.where(low, query, 0.0).astype(jnp.bfloat16)
        stack_ref[odd, :] = jnp.where(low, turned, 0.0).astype(jnp.bfloat16)
        stack_ref[even_grad, :] = jnp.where(low, 0.0, turned_grad).astype(jnp.bfloat16)
        stack_ref[odd_grad, :] = jnp.where(low, 0.0, grad).astype(jnp.bfloat16)
    dq_t_ref[...] = jnp.zeros_like(dq_t_ref)
    lse = lse_ref[0]
    delta = delta_ref[0]
    shape = (BLOCK, width)
    ahead = lax.broadcasted_iota(jnp.int32, shape, 0) - (
        lax.broadcasted_iota(jnp.int32, shape, 1) & (BLOCK - 1)
    )

    def some_slots(turn, carry):
        first = turn * slots_at_once
        places = [slot_ref[block, first + i] for i in range(slots_at_once)]
        limits = [limit_ref[block, first + i] for i in range(slots_at_once)]
        rows = [pl.ds(pl.multiple_of(place * BLOCK, BLOCK), BLOCK) for place in places]
        pair_rows = jnp.concatenate([table_ref[row, :] for row in rows], axis=0)
        both = lax.dot_general(
            pair_rows, stack_ref[...], (((1,), (1,)), ((), ())),
            preferred_element_type=jnp.float32,
        )
        allowed = jnp.concatenate([ahead <= limit for limit in limits], axis=0)
        powers = both[:, :width] * (score_scale * math.log2(math.e)) - lse
        probs = jnp.where(allowed, jnp.exp2(powers), 0.0)
        dscores = (probs * (both[:, width:] - delta)).astype(jnp.bfloat16)
        terms = jnp.concatenate([dscores, probs.astype(jnp.bfloat16)], axis=1)
        grads = jnp.dot(terms, stack_ref[...], preferred_element_type=jnp.float32)
        dq_t_ref[...] += lax.dot_general(
            pair_rows[:, :head_dim], dscores, (((0,), (0,)), ((), ())),
            preferred_element_type=jnp.float32,
        )
        for i, row in enumerate(rows):
            sums_ref[row, :] += grads[i * BLOCK:(i + 1) * BLOCK]
        return carry

    lax.fori_loop(0, rounds_ref[block], some_slots, 0)
    half = width // 2
    dq_t = dq_t_ref[...] * score_scale
    for pair in range(pairs):
        cols = slice(pair * BLOCK, (pair + 1) * BLOCK)
        odd_cols = slice(half + pair * BLOCK, half + (pair + 1) * BLOCK)
        both_heads = jnp.concatenate([dq_t[:, cols], dq_t[:, odd_cols]], axis=0)
        columns = slice(pair * 2 * head_dim, (pair + 1) * 2 * head_dim)
        dq_ref[:, columns] = both_heads.T.astype(jnp.bfloat16)

    @pl.when(block == pl.num_programs(0) - 1)
    def _():
        sums = sums_ref[...]
        low = lax.broadcasted_iota(jnp.int32, sums.shape, 1) < head_dim
        sums_ref[...] = jnp.where(low, sums * score_scale, sums)


def attention_backward(
    queries, cotangent, attended, log_sum, block_table, slot_index, chosen, my_rank
):
    tok_rows, width = queries.shape
    heads = log_sum.shape[1]
    head_dim = width // heads
    blocks, slot_count = chosen.shape
    slots_at_once = 4 if slot_count % 4 == 0 else 1
    listed = chosen >= 0
    own = my_rank * blocks + jnp.arange(blocks, dtype=jnp.int32)
    limits = jnp.where(listed, (own[:, None] - chosen) * BLOCK, -BLOCK)
    count = jnp.sum(listed.astype(jnp.int32), axis=1)
    rounds = (count + slots_at_once - 1) // slots_at_once
    deltas = jnp.sum(
        (cotangent.astype(jnp.float32) * attended.astype(jnp.float32)).reshape(
            tok_rows, heads, head_dim
        ),
        axis=-1,
    )
    table = block_table.reshape(-1, 2 * head_dim)
    step = lambda g, *_: (g, 0)
    row = lambda g, *_: (g, 0, 0)
    whole = lambda g, *_: (0, 0)
    query_gradient, sums = pl.pallas_call(
        functools.partial(attention_kernel, slots_at_once, head_dim),
        grid_spec=pltpu.PrefetchScalarGridSpec(
            num_scalar_prefetch=3,
            grid=(blocks,),
            in_specs=[
                pl.BlockSpec((BLOCK, width), step),
                pl.BlockSpec((BLOCK, width), step),
                pl.BlockSpec((1, 1, heads * BLOCK), row),
                pl.BlockSpec((1, 1, heads * BLOCK), row),
                pl.BlockSpec(table.shape, whole),
            ],
            out_specs=[
                pl.BlockSpec((BLOCK, width), step),
                pl.BlockSpec(table.shape, whole),
            ],
            scratch_shapes=[
                pltpu.VMEM((2 * heads * BLOCK, 2 * head_dim), jnp.bfloat16),
                pltpu.VMEM((head_dim, heads * BLOCK), jnp.float32),
            ],
        ),
        out_shape=[
            jax.ShapeDtypeStruct((tok_rows, width), jnp.bfloat16),
            jax.ShapeDtypeStruct(table.shape, jnp.float32),
        ],
        compiler_params=pltpu.CompilerParams(dimension_semantics=("arbitrary",)),
        cost_estimate=pl.CostEstimate(
            flops=10 * tok_rows * slot_count * BLOCK * width,
            bytes_accessed=4 * tok_rows * width * 2,
            transcendentals=tok_rows * heads * slot_count * BLOCK,
        ),
    )(
        slot_index, limits, rounds, queries, cotangent,
        by_parity(log_sum * math.log2(math.e), blocks, heads), by_parity(deltas, blocks, heads),
        table,
    )
    return query_gradient, sums.reshape(block_table.shape)


def shards(normed, queries, keys, values, attended, cotangent, log_sum, chosen):
    my_rank = lax.axis_index("kv")
    peer_count = lax.axis_size("kv")
    tok_rows = normed.shape[0]
    local_blocks = tok_rows // BLOCK
    head_dim = keys.shape[1]
    moved, mine = regroup_normed(normed)
    pairs_local = jnp.concatenate([keys, values], axis=1).reshape(local_blocks, BLOCK, 2 * head_dim)
    owners = chosen // local_blocks
    within = chosen % local_blocks
    listed = chosen >= 0
    remote = listed & (owners != my_rank)
    peer_ids = jnp.arange(peer_count, dtype=jnp.int32)
    matched = remote[:, :, None] & (owners[:, :, None] == peer_ids[None, None, :])
    wanted = jnp.max(jnp.where(matched, within[:, :, None] + 1, 0), axis=(0, 1))
    asked_for = (
        lax.all_to_all(
            wanted.reshape(peer_count, 1), "kv", split_axis=0, concat_axis=0, tiled=True
        )[:, 0]
        - 1
    )
    picked = jnp.maximum(asked_for, 0)
    outgoing = jnp.take(pairs_local, picked, axis=0)
    fetched = lax.all_to_all(outgoing, "kv", split_axis=0, concat_axis=0, tiled=True)
    block_table = jnp.concatenate([pairs_local, fetched], axis=0)
    slot_index = jnp.where(owners == my_rank, within, local_blocks + owners)
    slot_index = jnp.where(listed, slot_index, 0)
    query_gradient, block_sums = attention_backward(
        queries, cotangent, attended, log_sum, block_table, slot_index, chosen, my_rank
    )
    own_part = block_sums[:local_blocks]
    sent_back = block_sums[local_blocks:].astype(jnp.bfloat16)
    taken_by = (asked_for[:, None] == jnp.arange(local_blocks, dtype=jnp.int32)[None, :]).astype(
        jnp.float32
    )
    weight_grad = weight_gradient(moved, mine, query_gradient)
    returned = lax.all_to_all(sent_back, "kv", split_axis=0, concat_axis=0, tiled=True)
    totals = own_part + jnp.einsum(
        "sb,skc->bkc", taken_by, returned.astype(jnp.float32), precision=lax.Precision.HIGHEST
    )
    totals = sum_over_tp(totals)
    grad_keys = totals[:, :, :head_dim].reshape(tok_rows, head_dim)
    grad_values = totals[:, :, head_dim:].reshape(tok_rows, head_dim)
    return (query_gradient, grad_keys, grad_values, weight_grad)


def solution(mesh):
    placed = (
        P("kv", None),
        P("kv", "tp"),
        P("kv", None),
        P("kv", None),
        P("kv", "tp"),
        P("kv", "tp"),
        P("kv", "tp"),
        P("kv", None),
    )
    return jax.shard_map(
        shards,
        mesh=mesh,
        in_specs=placed,
        out_specs=(P("kv", "tp"), P("kv", None), P("kv", None), P("kv", "tp")),
        check_vma=False,
    )
```

```python
import functools
import math

import jax
import jax.numpy as jnp
from jax import lax
from jax.experimental import pallas as pl
from jax.experimental.pallas import tpu as pltpu

from jax.sharding import PartitionSpec as P

BLOCK = 64
STACK_UNROLL = 4
BLOCK_UNROLL = 2


def flat_perm(kv_of, tp_of=lambda core: core):
    kv_size, tp_size = lax.axis_size("kv"), lax.axis_size("tp")
    return [
        (kv * tp_size + tp, kv_of(kv) * tp_size + tp_of(tp))
        for kv in range(kv_size)
        for tp in range(tp_size)
    ]


def send(value, perm):
    return lax.ppermute(value, ("kv", "tp"), perm)


def group_size():
    kv_size = lax.axis_size("kv")
    return 4 if kv_size % 4 == 0 else 2 if kv_size % 2 == 0 else 1


def step_perm(step, size, stride):
    if size & (size - 1) == 0:
        return lambda kv: kv ^ (step * stride)
    base = size * stride
    return lambda kv: kv // base * base + (kv % base + step * stride) % base


def partner(index, step, size):
    return index ^ step if size & (size - 1) == 0 else (index + step) % size


def columns_of(normed, member, group, first, rows):
    kv_size = lax.axis_size("kv")
    width = normed.shape[1] // kv_size
    parts = [
        lax.dynamic_slice(normed, (first, (outer * group + member) * width), (rows, width))
        for outer in range(kv_size // group)
    ]
    return jnp.concatenate(parts, axis=1)


def regroup_normed(normed, share):
    group = group_size()
    member = lax.axis_index("kv") % group
    half = normed.shape[0] // 2
    pieces = [
        columns_of(normed, partner(member, step, group), group, share * half, half)
        for step in range(1, group)
    ]
    mine = [
        columns_of(normed, member, group, first * half, half) for first in (share, 1 - share)
    ]
    return pieces, jnp.concatenate(mine, axis=0)


def exchange_normed(pieces):
    group = group_size()
    got = [
        send(piece, flat_perm(step_perm(step, group, 1)))
        for step, piece in enumerate(pieces, start=1)
    ]
    other = send(jnp.stack(got), flat_perm(lambda kv: kv, lambda tp: tp ^ 1))
    return got, other


def gather_group(value):
    group = group_size()
    return [send(value, flat_perm(step_perm(step, group, 1))) for step in range(1, group)]


def plane_kernel(outer, group, place_ref, *refs):
    rights, mine_ref, others = refs[:group], refs[group], refs[group + 1:2 * group]
    other_ref, own_ref, pieces = refs[2 * group], refs[2 * group + 1], refs[2 * group + 2:]
    half = mine_ref.shape[0] // 2
    width = mine_ref.shape[1] // outer
    for step in range(outer):
        owner = partner(place_ref[0], step, outer)
        columns = pl.ds(pl.multiple_of(owner * width, width), width)
        total = jnp.dot(
            rights[0][...], mine_ref[:, columns], preferred_element_type=jnp.float32
        )
        for i in range(group - 1):
            total += jnp.dot(
                rights[i + 1][:, :half], others[i][:, columns],
                preferred_element_type=jnp.float32,
            )
            total += jnp.dot(
                rights[i + 1][:, half:], other_ref[i, :, columns],
                preferred_element_type=jnp.float32,
            )
        if step == 0:
            own_ref[...] = total
        else:
            pieces[step - 1][...] = total.astype(jnp.bfloat16)


def weight_gradient(mine, got, other, rights):
    group = group_size()
    outer = lax.axis_size("kv") // group
    place = lax.axis_index("kv") // group
    columns = rights[0].shape[0]
    width = mine.shape[1] // outer
    if width % 128 == 0:
        in_vmem = pl.BlockSpec(memory_space=pltpu.VMEM)
        own, *pieces = pl.pallas_call(
            functools.partial(plane_kernel, outer, group),
            in_specs=[pl.BlockSpec(memory_space=pltpu.SMEM)] + [in_vmem] * (2 * group + 1),
            out_specs=[in_vmem] * outer,
            out_shape=[jax.ShapeDtypeStruct((columns, width), jnp.float32)] + [
                jax.ShapeDtypeStruct((columns, width), jnp.bfloat16)
            ] * (outer - 1),
            cost_estimate=pl.CostEstimate(
                flops=2 * columns * mine.size * group,
                bytes_accessed=2 * group * mine.size,
                transcendentals=0,
            ),
        )(place.reshape(1).astype(jnp.int32), *rights, mine, *got, other)
    else:
        lefts = [mine]
        for i, piece in enumerate(got):
            lefts += [piece, other[i]]
        partial = jnp.dot(
            jnp.concatenate(rights, axis=1), jnp.concatenate(lefts, axis=0),
            preferred_element_type=jnp.float32,
        )
        own, *pieces = [
            lax.dynamic_slice_in_dim(partial, partner(place, step, outer) * width, width, axis=1)
            for step in range(outer)
        ]
        pieces = [piece.astype(jnp.bfloat16) for piece in pieces]
    terms = [own]
    for step, piece in enumerate(pieces, start=1):
        terms.append(send(piece, flat_perm(step_perm(step, outer, group))))
    return terms


def sum_over_tp(value):
    tp_size = lax.axis_size("tp")
    step = 1
    if tp_size & (tp_size - 1):
        return lax.psum(value, "tp")
    while step < tp_size:
        value = value + send(value, flat_perm(lambda kv: kv, lambda tp: tp ^ step))
        step *= 2
    return value


def attention_kernel(
    head_dim, first, last, part, share_ref, slot_ref, limit_ref, q_ref, d_ref, log_ref, sum_ref,
    table_ref, *rest,
):
    before_ref = None if first else rest[0]
    dq_ref, turned_ref, sums_ref, stack_ref, dq_t_ref, lse_ref, delta_ref = rest[-7:]
    blocks, slot_count = slot_ref.shape
    width = lse_ref.shape[2]
    half = width // 2
    wide = 2 * head_dim
    pairs = width // (2 * BLOCK)
    offset = part * pairs
    score_scale = head_dim ** (-0.5)
    low = lax.broadcasted_iota(jnp.int32, (BLOCK, wide), 1) < head_dim

    sums_ref[...] = jnp.zeros_like(sums_ref) if first else before_ref[...]

    def stack_heads(block, carry):
        rows = pl.ds(pl.multiple_of(block * BLOCK, BLOCK), BLOCK)
        for pair in range(pairs):
            columns = pl.ds((offset + pair) * wide, wide)
            query = q_ref[rows, columns].astype(jnp.float32)
            grad = d_ref[rows, columns].astype(jnp.float32)
            turned = pltpu.roll(query, head_dim, 1)
            turned_grad = pltpu.roll(grad, head_dim, 1)
            for place, value in enumerate((
                jnp.where(low, query, 0.0), jnp.where(low, turned, 0.0),
                jnp.where(low, 0.0, turned_grad), jnp.where(low, 0.0, grad),
            )):
                stack_ref[block, pl.ds((place * pairs + pair) * BLOCK, BLOCK), :] = value.astype(
                    jnp.bfloat16
                )
        return carry

    lax.fori_loop(0, blocks, stack_heads, 0, unroll=min(blocks, STACK_UNROLL))
    for block in range(blocks):
        rows = slice(block * BLOCK, (block + 1) * BLOCK)
        for parity in range(2):
            for pair in range(pairs):
                head = 2 * (offset + pair) + parity
                place = slice((parity * pairs + pair) * BLOCK, (parity * pairs + pair + 1) * BLOCK)
                lse_ref[block, :, place] = log_ref[head:head + 1, rows] * math.log2(math.e)
                delta_ref[block, :, place] = sum_ref[head:head + 1, rows]
    shape = (BLOCK, width)
    ahead = lax.broadcasted_iota(jnp.int32, shape, 0) - (
        lax.broadcasted_iota(jnp.int32, shape, 1) & (BLOCK - 1)
    )

    def one_block(block, carry):
        stack = stack_ref[block]
        places = [slot_ref[block, i] for i in range(slot_count)]
        limits = [limit_ref[block, i] for i in range(slot_count)]
        rows = [pl.ds(pl.multiple_of(place * BLOCK, BLOCK), BLOCK) for place in places]
        pair_rows = jnp.concatenate([table_ref[row, :] for row in rows], axis=0)
        both = lax.dot_general(
            pair_rows, stack, (((1,), (1,)), ((), ())), preferred_element_type=jnp.float32
        )
        allowed = jnp.concatenate([ahead <= limit for limit in limits], axis=0)
        powers = both[:, :width] * (score_scale * math.log2(math.e)) - lse_ref[block]
        probs = jnp.where(allowed, jnp.exp2(powers), 0.0)
        dscores = (probs * (both[:, width:] - delta_ref[block])).astype(jnp.bfloat16)
        terms = jnp.concatenate([dscores, probs.astype(jnp.bfloat16)], axis=1)
        grads = jnp.dot(terms, stack, preferred_element_type=jnp.float32)
        dq_t_ref[block] = score_scale * lax.dot_general(
            pair_rows[:, :head_dim], dscores, (((0,), (0,)), ((), ())),
            preferred_element_type=jnp.float32,
        )
        for i, row in enumerate(rows):
            sums_ref[row, :] += grads[i * BLOCK:(i + 1) * BLOCK]
        return carry

    lax.fori_loop(0, blocks, one_block, 0, unroll=BLOCK_UNROLL)

    def write_two(turn, carry):
        first_block = 2 * turn
        to = lax.rem(first_block + share_ref[0] * (blocks // 2), blocks) * BLOCK
        for pair in range(pairs):
            cols = slice(pair * BLOCK, (pair + 1) * BLOCK)
            odd_cols = slice(half + pair * BLOCK, half + (pair + 1) * BLOCK)
            heads_t = []
            for block in (first_block, first_block + 1):
                heads_t.append(jnp.concatenate(
                    [dq_t_ref[block, :, cols], dq_t_ref[block, :, odd_cols]], axis=0
                ))
            both_t = jnp.concatenate(heads_t, axis=1)
            turned_ref[pl.ds(pair * wide, wide), pl.ds(pl.multiple_of(to, 2 * BLOCK), 2 * BLOCK)] = (
                both_t.astype(jnp.bfloat16)
            )
            dq_ref[
                pl.ds(pl.multiple_of(first_block * BLOCK, 2 * BLOCK), 2 * BLOCK),
                pl.ds(pair * wide, wide),
            ] = both_t.T.astype(jnp.bfloat16)
        return carry

    lax.fori_loop(0, blocks // 2, write_two, 0, unroll=min(blocks // 2, STACK_UNROLL))
    if last:
        sums = sums_ref[...]
        low_columns = lax.broadcasted_iota(jnp.int32, sums.shape, 1) < head_dim
        sums_ref[...] = jnp.where(low_columns, sums * score_scale, sums)


def attention_backward(
    queries, cotangent, log_sum, deltas, table, share, slot_index, limits, part, parts, before
):
    tok_rows, width = queries.shape
    blocks, slot_count = slot_index.shape
    head_dim = table.shape[1] // 2
    width //= parts
    heads = width // head_dim
    first, last = part == 0, part == parts - 1
    in_smem = pl.BlockSpec(memory_space=pltpu.SMEM)
    in_vmem = pl.BlockSpec(memory_space=pltpu.VMEM)
    return pl.pallas_call(
        functools.partial(attention_kernel, head_dim, first, last, part),
        in_specs=[in_smem] * 3 + [in_vmem] * (5 if first else 6),
        out_specs=[in_vmem] * 3,
        scratch_shapes=[
            pltpu.VMEM((blocks, 2 * heads * BLOCK, 2 * head_dim), jnp.bfloat16),
            pltpu.VMEM((blocks, head_dim, heads * BLOCK), jnp.float32),
            pltpu.VMEM((blocks, 1, heads * BLOCK), jnp.float32),
            pltpu.VMEM((blocks, 1, heads * BLOCK), jnp.float32),
        ],
        out_shape=[
            jax.ShapeDtypeStruct((tok_rows, width), jnp.bfloat16),
            jax.ShapeDtypeStruct((width, tok_rows), jnp.bfloat16),
            jax.ShapeDtypeStruct(table.shape, jnp.float32),
        ],
        cost_estimate=pl.CostEstimate(
            flops=10 * tok_rows * slot_count * BLOCK * width,
            bytes_accessed=4 * tok_rows * width * 2,
            transcendentals=tok_rows * heads * slot_count * BLOCK,
        ),
    )(
        share.reshape(1), slot_index, limits, queries, cotangent, log_sum, deltas, table,
        *(() if first else (before,)),
    )


def shards(normed, queries, keys, values, attended, cotangent, log_sum, chosen):
    my_rank = lax.axis_index("kv")
    peer_count = lax.axis_size("kv")
    tok_rows = normed.shape[0]
    local_blocks = tok_rows // BLOCK
    head_dim = keys.shape[1]
    pairs_local = jnp.concatenate([keys, values], axis=1).reshape(local_blocks, BLOCK, 2 * head_dim)
    owners = chosen // local_blocks
    within = chosen % local_blocks
    listed = chosen >= 0
    remote = listed & (owners != my_rank)
    peer_ids = jnp.arange(peer_count, dtype=jnp.int32)
    matched = remote[:, :, None] & (owners[:, :, None] == peer_ids[None, None, :])
    wanted = jnp.max(jnp.where(matched, within[:, :, None] + 1, 0), axis=(0, 1))
    asked_for = (
        lax.all_to_all(
            wanted.reshape(peer_count, 1), "kv", split_axis=0, concat_axis=0, tiled=True
        )[:, 0]
        - 1
    )
    picked = jnp.maximum(asked_for, 0)
    outgoing = jnp.take(pairs_local, picked, axis=0)
    outgoing, normed = lax.optimization_barrier((outgoing, normed))
    fetched = lax.all_to_all(outgoing, "kv", split_axis=0, concat_axis=0, tiled=True)
    share = (lax.axis_index("tp") % 2).astype(jnp.int32)
    pieces, mine = regroup_normed(normed, share)
    got, other = exchange_normed(pieces)
    block_table = jnp.concatenate([pairs_local, fetched], axis=0)
    slot_index = jnp.where(owners == my_rank, within, local_blocks + owners)
    slot_index = jnp.where(listed, slot_index, 0)
    heads = log_sum.shape[1]
    parts = 2 if heads % 4 == 0 else 1
    own = my_rank * local_blocks + jnp.arange(local_blocks, dtype=jnp.int32)
    limits = jnp.where(listed, (own[:, None] - chosen) * BLOCK, -BLOCK)
    head_of = jnp.arange(heads * head_dim, dtype=jnp.int32) // head_dim
    deltas = lax.dot_general(
        (jnp.arange(heads, dtype=jnp.int32)[:, None] == head_of[None, :]).astype(jnp.float32),
        cotangent.astype(jnp.float32) * attended.astype(jnp.float32),
        (((1,), (1,)), ((), ())), precision=lax.Precision.HIGHEST,
    )
    table = block_table.reshape(-1, 2 * head_dim)
    sums = None
    gradients, rights = [], []
    for part in range(parts):
        gradient, turned, sums = attention_backward(
            queries, cotangent, log_sum.T, deltas, table, share, slot_index, limits, part,
            parts, sums,
        )
        gradients.append(gradient)
        rights.append([turned] + gather_group(turned))
    query_gradient = jnp.concatenate(gradients, axis=1)
    block_sums = sums.reshape(block_table.shape)
    own_part = block_sums[:local_blocks]
    sent_back = block_sums[local_blocks:].astype(jnp.bfloat16)
    taken_by = (asked_for[:, None] == jnp.arange(local_blocks, dtype=jnp.int32)[None, :]).astype(
        jnp.float32
    )
    terms = [weight_gradient(mine, got, other, right) for right in rights]
    weight_grad = jnp.concatenate(
        [sum(term.astype(jnp.float32) for term in some) for some in terms], axis=0
    ).T
    returned = lax.all_to_all(sent_back, "kv", split_axis=0, concat_axis=0, tiled=True)
    totals = own_part + jnp.einsum(
        "sb,skc->bkc", taken_by, returned.astype(jnp.float32), precision=lax.Precision.HIGHEST
    )
    totals = sum_over_tp(totals)
    grad_keys = totals[:, :, :head_dim].reshape(tok_rows, head_dim)
    grad_values = totals[:, :, head_dim:].reshape(tok_rows, head_dim)
    return (query_gradient, grad_keys, grad_values, weight_grad)


def solution(mesh):
    placed = (
        P("kv", None),
        P("kv", "tp"),
        P("kv", None),
        P("kv", None),
        P("kv", "tp"),
        P("kv", "tp"),
        P("kv", "tp"),
        P("kv", None),
    )
    return jax.shard_map(
        shards,
        mesh=mesh,
        in_specs=placed,
        out_specs=(P("kv", "tp"), P("kv", None), P("kv", None), P("kv", "tp")),
        check_vma=False,
    )
```

```python
import functools
import math

import jax
import jax.numpy as jnp
from jax import lax
from jax.experimental import pallas as pl
from jax.experimental.pallas import tpu as pltpu

from jax.sharding import PartitionSpec as P

BLOCK = 64
ATTEND_VMEM = 28 * 2**20
PLANE_VMEM = 16 * 2**20
STACK_UNROLL = 4
BLOCK_UNROLL = 2


def flat_perm(kv_of, tp_of=lambda core: core):
    kv_size, tp_size = lax.axis_size("kv"), lax.axis_size("tp")
    return [
        (kv * tp_size + tp, kv_of(kv) * tp_size + tp_of(tp))
        for kv in range(kv_size)
        for tp in range(tp_size)
    ]


def send(value, perm):
    return lax.ppermute(value, ("kv", "tp"), perm)


def group_size():
    kv_size = lax.axis_size("kv")
    return 4 if kv_size % 4 == 0 else 2 if kv_size % 2 == 0 else 1


def step_perm(step, size, stride):
    if size & (size - 1) == 0:
        return lambda kv: kv ^ (step * stride)
    base = size * stride
    return lambda kv: kv // base * base + (kv % base + step * stride) % base


def partner(index, step, size):
    return index ^ step if size & (size - 1) == 0 else (index + step) % size


def columns_of(normed, member, group, first, rows):
    kv_size = lax.axis_size("kv")
    width = normed.shape[1] // kv_size
    parts = [
        lax.dynamic_slice(normed, (first, (outer * group + member) * width), (rows, width))
        for outer in range(kv_size // group)
    ]
    return jnp.concatenate(parts, axis=1)


def regroup_normed(normed, share):
    group = group_size()
    member = lax.axis_index("kv") % group
    half = normed.shape[0] // 2
    pieces = [
        columns_of(normed, partner(member, step, group), group, share * half, half)
        for step in range(1, group)
    ]
    mine = [columns_of(normed, member, group, first * half, half) for first in (share, 1 - share)]
    mine = jnp.concatenate(mine, axis=0)
    return pieces, mine


def exchange_normed(pieces):
    group = group_size()
    got = [
        send(piece, flat_perm(step_perm(step, group, 1)))
        for step, piece in enumerate(pieces, start=1)
    ]
    other = [send(piece, flat_perm(lambda kv: kv, lambda tp: tp ^ 1)) for piece in got]
    return got, other


def gather_group(value):
    group = group_size()
    return [send(value, flat_perm(step_perm(step, group, 1))) for step in range(1, group)]


def plane_kernel(outer, group, place_ref, *refs):
    rights, mine_ref = refs[:group], refs[group]
    others, swapped = refs[group + 1:2 * group], refs[2 * group:3 * group - 1]
    own_ref, pieces = refs[3 * group - 1], refs[3 * group:]
    width = mine_ref.shape[1] // outer
    right = jnp.concatenate([ref[...] for ref in rights], axis=1)
    for step in range(outer):
        owner = partner(place_ref[0], step, outer)
        columns = pl.ds(pl.multiple_of(owner * width, width), width)
        left = [mine_ref[:, columns]]
        for first, second in zip(others, swapped):
            left += [first[:, columns], second[:, columns]]
        total = jnp.dot(
            right, jnp.concatenate(left, axis=0), preferred_element_type=jnp.float32
        )
        if step == 0:
            own_ref[...] = total
        else:
            pieces[step - 1][...] = total.astype(jnp.bfloat16)


def weight_gradient(mine, got, other, rights):
    group = group_size()
    outer = lax.axis_size("kv") // group
    place = lax.axis_index("kv") // group
    columns = rights[0].shape[0]
    width = mine.shape[1] // outer
    if width % 128 == 0:
        in_vmem = pl.BlockSpec(memory_space=pltpu.VMEM)
        own, *pieces = pl.pallas_call(
            functools.partial(plane_kernel, outer, group),
            in_specs=[pl.BlockSpec(memory_space=pltpu.SMEM)] + [in_vmem] * (3 * group - 1),
            out_specs=[in_vmem] * outer,
            out_shape=[jax.ShapeDtypeStruct((columns, width), jnp.float32)] + [
                jax.ShapeDtypeStruct((columns, width), jnp.bfloat16)
            ] * (outer - 1),
            compiler_params=pltpu.CompilerParams(vmem_limit_bytes=PLANE_VMEM),
            cost_estimate=pl.CostEstimate(
                flops=2 * columns * mine.size * group,
                bytes_accessed=2 * group * mine.size,
                transcendentals=0,
            ),
        )(place.reshape(1).astype(jnp.int32), *rights, mine, *got, *other)
    else:
        lefts = [mine]
        for i, piece in enumerate(got):
            lefts += [piece, other[i]]
        partial = jnp.dot(
            jnp.concatenate(rights, axis=1), jnp.concatenate(lefts, axis=0),
            preferred_element_type=jnp.float32,
        )
        own, *pieces = [
            lax.dynamic_slice_in_dim(partial, partner(place, step, outer) * width, width, axis=1)
            for step in range(outer)
        ]
        pieces = [piece.astype(jnp.bfloat16) for piece in pieces]
    terms = [own]
    for step, piece in enumerate(pieces, start=1):
        terms.append(send(piece, flat_perm(step_perm(step, outer, group))))
    return terms


def attention_kernel(
    head_dim, first, last, part, share_ref, slot_ref, limit_ref, q_ref, d_ref, log_ref, sum_ref,
    table_ref, *rest,
):
    before_ref = None if first else rest[0]
    sums_ref, stack_ref, dq_t_ref, lse_ref, delta_ref = rest[-5:]
    dq_ref, turned_ref = rest[:2] if first else rest[1:3]
    blocks, slot_count = slot_ref.shape
    width = lse_ref.shape[2]
    half = width // 2
    wide = 2 * head_dim
    pairs = width // (2 * BLOCK)
    offset = part * pairs
    score_scale = head_dim ** (-0.5)
    low = lax.broadcasted_iota(jnp.int32, (BLOCK, wide), 1) < head_dim

    sums_ref[...] = jnp.zeros_like(sums_ref) if first else before_ref[...]

    def stack_heads(block, carry):
        rows = pl.ds(pl.multiple_of(block * BLOCK, BLOCK), BLOCK)
        for pair in range(pairs):
            columns = pl.ds((offset + pair) * wide, wide)
            query = q_ref[rows, columns].astype(jnp.float32)
            grad = d_ref[rows, columns].astype(jnp.float32)
            turned = pltpu.roll(query, head_dim, 1)
            turned_grad = pltpu.roll(grad, head_dim, 1)
            for place, value in enumerate((
                jnp.where(low, query, 0.0), jnp.where(low, turned, 0.0),
                jnp.where(low, 0.0, turned_grad), jnp.where(low, 0.0, grad),
            )):
                stack_ref[block, pl.ds((place * pairs + pair) * BLOCK, BLOCK), :] = value.astype(
                    jnp.bfloat16
                )
        return carry

    lax.fori_loop(0, blocks, stack_heads, 0, unroll=min(blocks, STACK_UNROLL))
    for block in range(blocks):
        rows = slice(block * BLOCK, (block + 1) * BLOCK)
        for parity in range(2):
            for pair in range(pairs):
                head = 2 * (offset + pair) + parity
                place = slice((parity * pairs + pair) * BLOCK, (parity * pairs + pair + 1) * BLOCK)
                lse_ref[block, :, place] = log_ref[head:head + 1, rows] * math.log2(math.e)
                delta_ref[block, :, place] = sum_ref[head:head + 1, rows]
    shape = (BLOCK, width)
    ahead = lax.broadcasted_iota(jnp.int32, shape, 0) - (
        lax.broadcasted_iota(jnp.int32, shape, 1) & (BLOCK - 1)
    )

    def one_block(block, carry):
        stack = stack_ref[block]
        places = [slot_ref[block, i] for i in range(slot_count)]
        limits = [limit_ref[block, i] for i in range(slot_count)]
        rows = [pl.ds(pl.multiple_of(place * BLOCK, BLOCK), BLOCK) for place in places]
        pair_rows = jnp.concatenate([table_ref[row, :] for row in rows], axis=0)
        both = lax.dot_general(
            pair_rows, stack, (((1,), (1,)), ((), ())), preferred_element_type=jnp.float32
        )
        allowed = jnp.concatenate([ahead <= limit for limit in limits], axis=0)
        powers = both[:, :width] * (score_scale * math.log2(math.e)) - lse_ref[block]
        probs = jnp.where(allowed, jnp.exp2(powers), 0.0)
        dscores = (probs * (both[:, width:] - delta_ref[block])).astype(jnp.bfloat16)
        terms = jnp.concatenate([dscores, probs.astype(jnp.bfloat16)], axis=1)
        grads = jnp.dot(terms, stack, preferred_element_type=jnp.float32)
        dq_t_ref[block] = score_scale * lax.dot_general(
            pair_rows[:, :head_dim], dscores, (((0,), (0,)), ((), ())),
            preferred_element_type=jnp.float32,
        )
        for i, row in enumerate(rows):
            sums_ref[row, :] += grads[i * BLOCK:(i + 1) * BLOCK]
        return carry

    lax.fori_loop(0, blocks, one_block, 0, unroll=BLOCK_UNROLL)

    def write_two(turn, carry):
        first_block = 2 * turn
        to = lax.rem(first_block + share_ref[0] * (blocks // 2), blocks) * BLOCK
        for pair in range(pairs):
            cols = slice(pair * BLOCK, (pair + 1) * BLOCK)
            odd_cols = slice(half + pair * BLOCK, half + (pair + 1) * BLOCK)
            heads_t = []
            for block in (first_block, first_block + 1):
                heads_t.append(jnp.concatenate(
                    [dq_t_ref[block, :, cols], dq_t_ref[block, :, odd_cols]], axis=0
                ))
            both_t = jnp.concatenate(heads_t, axis=1)
            turned_ref[pl.ds(pair * wide, wide), pl.ds(pl.multiple_of(to, 2 * BLOCK), 2 * BLOCK)] = (
                both_t.astype(jnp.bfloat16)
            )
            dq_ref[
                pl.ds(pl.multiple_of(first_block * BLOCK, 2 * BLOCK), 2 * BLOCK),
                pl.ds(pair * wide, wide),
            ] = both_t.T.astype(jnp.bfloat16)
        return carry

    lax.fori_loop(0, blocks // 2, write_two, 0, unroll=min(blocks // 2, STACK_UNROLL))
    if last:
        kept_ref, sent_ref = rest[-7:-5]
        kept = kept_ref.shape[0]
        low_columns = lax.broadcasted_iota(jnp.int32, (1, wide), 1) < head_dim
        scales = jnp.where(low_columns, score_scale, 1.0)
        kept_ref[...] = sums_ref[:kept] * scales
        sent_ref[...] = (sums_ref[kept:] * scales).astype(jnp.bfloat16)


def attention_backward(
    queries, cotangent, log_sum, deltas, table, share, slot_index, limits, part, parts, before
):
    tok_rows, width = queries.shape
    blocks, slot_count = slot_index.shape
    head_dim = table.shape[1] // 2
    width //= parts
    heads = width // head_dim
    first, last = part == 0, part == parts - 1
    in_smem = pl.BlockSpec(memory_space=pltpu.SMEM)
    in_vmem = pl.BlockSpec(memory_space=pltpu.VMEM)
    return pl.pallas_call(
        functools.partial(attention_kernel, head_dim, first, last, part),
        in_specs=[in_smem] * 3 + [in_vmem] * (5 if first else 6),
        out_specs=[in_vmem] * (4 if last else 3),
        scratch_shapes=([pltpu.VMEM(table.shape, jnp.float32)] if last else []) + [
            pltpu.VMEM((blocks, 2 * heads * BLOCK, 2 * head_dim), jnp.bfloat16),
            pltpu.VMEM((blocks, head_dim, heads * BLOCK), jnp.float32),
            pltpu.VMEM((blocks, 1, heads * BLOCK), jnp.float32),
            pltpu.VMEM((blocks, 1, heads * BLOCK), jnp.float32),
        ],
        out_shape=[
            jax.ShapeDtypeStruct((tok_rows, width), jnp.bfloat16),
            jax.ShapeDtypeStruct((width, tok_rows), jnp.bfloat16),
        ] + ([
            jax.ShapeDtypeStruct((blocks * BLOCK, 2 * head_dim), jnp.float32),
            jax.ShapeDtypeStruct((table.shape[0] - blocks * BLOCK, 2 * head_dim), jnp.bfloat16),
        ] if last else [jax.ShapeDtypeStruct(table.shape, jnp.float32)]),
        compiler_params=pltpu.CompilerParams(vmem_limit_bytes=ATTEND_VMEM),
        cost_estimate=pl.CostEstimate(
            flops=10 * tok_rows * slot_count * BLOCK * width,
            bytes_accessed=4 * tok_rows * width * 2,
            transcendentals=tok_rows * heads * slot_count * BLOCK,
        ),
    )(
        share.reshape(1), slot_index, limits, queries, cotangent, log_sum, deltas, table,
        *(() if first else (before,)),
    )


def shards(normed, queries, keys, values, attended, cotangent, log_sum, chosen):
    my_rank = lax.axis_index("kv")
    peer_count = lax.axis_size("kv")
    tok_rows = normed.shape[0]
    local_blocks = tok_rows // BLOCK
    head_dim = keys.shape[1]
    pairs_local = jnp.concatenate([keys, values], axis=1).reshape(local_blocks, BLOCK, 2 * head_dim)
    owners = chosen // local_blocks
    within = chosen % local_blocks
    listed = chosen >= 0
    remote = listed & (owners != my_rank)
    peer_ids = jnp.arange(peer_count, dtype=jnp.int32)
    matched = remote[:, :, None] & (owners[:, :, None] == peer_ids[None, None, :])
    wanted = jnp.max(jnp.where(matched, within[:, :, None] + 1, 0), axis=(0, 1))
    asked_for = (
        lax.all_to_all(
            wanted.reshape(peer_count, 1), "kv", split_axis=0, concat_axis=0, tiled=True
        )[:, 0]
        - 1
    )
    picked = jnp.maximum(asked_for, 0)
    outgoing = jnp.take(pairs_local, picked, axis=0)
    fetched = lax.all_to_all(outgoing, "kv", split_axis=0, concat_axis=0, tiled=True)
    share = (lax.axis_index("tp") % 2).astype(jnp.int32)
    pieces, mine = regroup_normed(normed, share)
    got, other = exchange_normed(pieces)
    block_table = jnp.concatenate([pairs_local, fetched], axis=0)
    slot_index = jnp.where(owners == my_rank, within, local_blocks + owners)
    slot_index = jnp.where(listed, slot_index, 0)
    heads = log_sum.shape[1]
    parts = 2 if heads % 4 == 0 else 1
    own = my_rank * local_blocks + jnp.arange(local_blocks, dtype=jnp.int32)
    limits = jnp.where(listed, (own[:, None] - chosen) * BLOCK, -BLOCK)
    head_of = jnp.arange(heads * head_dim, dtype=jnp.int32) // head_dim
    deltas = lax.dot_general(
        (jnp.arange(heads, dtype=jnp.int32)[:, None] == head_of[None, :]).astype(jnp.float32),
        cotangent.astype(jnp.float32) * attended.astype(jnp.float32),
        (((1,), (1,)), ((), ())), precision=lax.Precision.HIGHEST,
    )
    table = block_table.reshape(-1, 2 * head_dim)
    sums = None
    gradients, rights = [], []
    for part in range(parts):
        gradient, turned, *sums = attention_backward(
            queries, cotangent, log_sum.T, deltas, table, share, slot_index, limits, part,
            parts, None if part == 0 else sums[0],
        )
        gradients.append(gradient)
        rights.append([turned] + gather_group(turned))
    query_gradient = jnp.concatenate(gradients, axis=1)
    own_part = sums[0].reshape(local_blocks, BLOCK, 2 * head_dim)
    sent_back = sums[1].reshape(peer_count, BLOCK, 2 * head_dim)
    taken_by = (asked_for[:, None] == jnp.arange(local_blocks, dtype=jnp.int32)[None, :]).astype(
        jnp.float32
    )
    terms = [weight_gradient(mine, got, other, right) for right in rights]
    weight_grad = jnp.concatenate(
        [sum(term.astype(jnp.float32) for term in some) for some in terms], axis=0
    ).T
    returned = lax.all_to_all(sent_back, "kv", split_axis=0, concat_axis=0, tiled=True)
    totals = own_part + jnp.einsum(
        "sb,skc->bkc", taken_by, returned.astype(jnp.float32), precision=lax.Precision.HIGHEST
    )
    tp_size = lax.axis_size("tp")
    step = 2
    while step < tp_size:
        totals = totals + send(totals, flat_perm(lambda kv: kv, lambda tp: tp ^ step))
        step *= 2
    received = send(totals, flat_perm(lambda kv: kv, lambda tp: tp ^ 1))
    totals = (totals + received).reshape(tok_rows, 2 * head_dim)
    grad_keys = totals[:, :head_dim]
    grad_values = totals[:, head_dim:]
    return (query_gradient, grad_keys, grad_values, weight_grad)


def solution(mesh):
    placed = (
        P("kv", None),
        P("kv", "tp"),
        P("kv", None),
        P("kv", None),
        P("kv", "tp"),
        P("kv", "tp"),
        P("kv", "tp"),
        P("kv", None),
    )
    return jax.shard_map(
        shards,
        mesh=mesh,
        in_specs=placed,
        out_specs=(P("kv", "tp"), P("kv", None), P("kv", None), P("kv", "tp")),
        check_vma=False,
    )
```
